32 devices in a mesh: grp: 2 (over x), tp: 16 (over z, y, core).
Axes of the slice: x: 2, y: 2, z: 4, core: 2. Of those that a mesh axis runs over, the one named last changes fastest.
Arguments:
- tokens: bfloat16 [160, 2048], P('grp', 'tp'), parts along dimension 0, may hold values from -6 to 6
- lengths: int32 [160], P('grp'), parts along dimension 0, may hold values from 1 to 4096, 81920 in all
- cell_memory: float32 [2, 160, 2048, 256], P(None, 'grp', 'tp'), parts along dimension 1, may hold values from -0.6 to 0.6
- key_sums: float32 [2, 160, 2048], P(None, 'grp', 'tp'), parts along dimension 1, may hold values from -3 to 3
- stabilizer: float32 [2, 160, 8], P(None, 'grp'), parts along dimension 1, may hold values from -3 to 1
- norm_gain: bfloat16 [2, 2048], replicated, may hold values from 0.099609375 to 1.8984375
- query_weight: bfloat16 [2, 2048, 2048], P(None, None, 'tp'), may hold values from -0.125 to 0.125
- key_weight: bfloat16 [2, 2048, 2048], P(None, None, 'tp'), may hold values from -0.125 to 0.125
- value_weight: bfloat16 [2, 2048, 2048], P(None, None, 'tp'), may hold values from -0.125 to 0.125
- outgate_weight: bfloat16 [2, 2048, 2048], P(None, None, 'tp'), may hold values from -0.125 to 0.125
- ingate_weight: bfloat16 [2, 2048, 8], replicated, may hold values from -0.125 to 0.125
- forget_weight: bfloat16 [2, 2048, 8], replicated, may hold values from -0.125 to 0.125
- ingate_bias: float32 [2, 8], replicated, may hold values from -3 to 3
- forget_bias: float32 [2, 8], replicated, may hold values from -1 to 4
- forget_slope: float32 [2, 8], replicated, may hold values from -3 to 3
- head_gain: bfloat16 [2, 2048], P(None, 'tp'), may hold values from 0.099609375 to 1.8984375
- output_weight: bfloat16 [2, 2048, 2048], P(None, None, 'tp'), may hold values from -0.125 to 0.125
Outputs:
- new_tokens: bfloat16 [160, 2048], P('grp', 'tp'), parts along dimension 0
- new_memory: float32 [2, 160, 2048, 256], P(None, 'grp', 'tp'), parts along dimension 1
- new_key_sums: float32 [2, 160, 2048], P(None, 'grp', 'tp'), parts along dimension 1
- new_stabilizer: float32 [2, 160, 8], P(None, 'grp'), parts along dimension 1
The draws below stay inside these ranges and needn't reach their ends.
There are 2 independent parts, one for each index of `grp`. The reference program is written for one: setup_inputs(seed, part) draws one part's arguments, and reference() takes and returns one part's arrays. A program takes and returns all parts, laid end to end along the dimension named above; an argument that names none is the same for every part. Nothing has to cross between parts.
Inputs may be any that keep to these rules, and one draw needn't show every extreme that they name: Each part's 80 lengths sum to 81920, and the largest is exactly 4096.
All inputs are finite; a program needn't handle non-finite values.
Results may differ from the reference program's by a relative error of at most 0.018.
Values may be sent and summed in bfloat16 or wider, within the bound.
No kernel may reach another device: no remote copies, remote signals or barrier semaphores. Data moves between devices by JAX's collectives and lax.ppermute only.
A program may use at most 128 MiB of HBM per device.

```python
import math
import jax
import jax.numpy as jnp
import numpy as np
from jax import lax

HEADS = 8
HEAD = 256
D = 2048
BATCH = 80
BLOCKS = 2
MEANLEN = 1024
MAXLEN = 4096


def shard_levels(stream_key, dims, shards, low, high):
    gain, own = 1.0, jax.random.fold_in(stream_key, 6)
    for dim, parts in shards:
        heights = jnp.exp(jax.random.uniform(jax.random.fold_in(own, dim), (parts,), jnp.float32, low / len(shards), high / len(shards)))
        gain = gain * jnp.repeat(heights, dims[dim] // parts).reshape([-1 if axis == dim else 1 for axis in range(len(dims))])
    return gain


def split_up(count, total, most, skew):
    portions = [(1 << 20) // math.isqrt(standing ** skew) + 1 for standing in range(2, count + 1)]
    rest, given = total - most - (count - 1), [1] * (count - 1)
    while rest > 0:
        movable = [i for i in range(count - 1) if given[i] < most]
        pool, budget = sum([portions[i] for i in movable]), rest
        for i in movable:
            addition = min(most - given[i], max(1, budget * portions[i] // pool), rest)
            given[i] = given[i] + addition
            rest = rest - addition
    return np.array([most] + given)


def uneven_parts(own_key, amount, total, reach, slope):
    if amount == 2:
        one = jax.random.randint(own_key, (), max(1, total - reach), min(reach, total - 1) + 1)
        return jnp.stack([one, total - one])
    sizes = jnp.asarray(split_up(amount, total, reach, slope), jnp.int32)
    pairs = (amount - 1) // 2
    donor, taker = sizes[1:1 + 2 * pairs:2], sizes[2:2 + 2 * pairs:2]
    margin = jnp.minimum(donor - 1, reach - taker)
    moved = jax.random.randint(jax.random.fold_in(own_key, 1), (pairs,), 0, 1 << 20) % (margin + 1)
    sizes = sizes.at[1:1 + 2 * pairs:2].set(donor - moved).at[2:2 + 2 * pairs:2].set(taker + moved)
    return sizes[jax.random.permutation(jax.random.fold_in(own_key, 2), amount)]


def scatter_about(stream_key, dims, width, reach, cuts=(), held_as=jnp.bfloat16):
    result = width * jax.random.normal(stream_key, dims, jnp.float32)
    if cuts:
        result = result * shard_levels(stream_key, dims, cuts, -0.22, 0.18)
    return jnp.clip(result, -reach, reach).astype(held_as)


def setup_inputs(seed: int = 0, part: int = 0) -> dict:
    streams_of = jax.random.split(jax.random.key(seed), 18)
    own_keys = jax.random.split(jax.random.fold_in(streams_of[17], part), 18)
    tokens = scatter_about(own_keys[0], (BATCH, D), 1.0, 6.0, ((1, 16),))
    lengths = uneven_parts(own_keys[1], BATCH, BATCH * MEANLEN, MAXLEN, 2).astype(jnp.int32)
    cell_memory = scatter_about(own_keys[2], (BLOCKS, BATCH, D, HEAD), 0.1, 0.6, ((2, 16),), jnp.float32)
    key_sums = scatter_about(own_keys[3], (BLOCKS, BATCH, D), 0.5, 3.0, ((2, 16),), jnp.float32)
    stabilizer = jnp.clip(jax.random.uniform(own_keys[4], (BLOCKS, BATCH, HEADS), jnp.float32, -3.0, 1.0), -3.0, 1.0)
    norm_gain = jnp.clip(1.0 + 0.18 * jax.random.normal(streams_of[5], (BLOCKS, D), jnp.float32), 0.099609375, 1.8984375).astype(jnp.bfloat16)
    query_weight = scatter_about(streams_of[6], (BLOCKS, D, D), D ** -0.5, 0.125, ((2, 16),))
    key_weight = scatter_about(streams_of[7], (BLOCKS, D, D), D ** -0.5, 0.125, ((2, 16),))
    value_weight = scatter_about(streams_of[8], (BLOCKS, D, D), D ** -0.5, 0.125, ((2, 16),))
    outgate_weight = scatter_about(streams_of[9], (BLOCKS, D, D), D ** -0.5, 0.125, ((2, 16),))
    ingate_weight = scatter_about(streams_of[10], (BLOCKS, D, HEADS), D ** -0.5, 0.125)
    forget_weight = scatter_about(streams_of[11], (BLOCKS, D, HEADS), D ** -0.5, 0.125)
    ingate_bias = scatter_about(streams_of[12], (BLOCKS, HEADS), 1.0, 3.0, (), jnp.float32)
    forget_bias = jnp.clip(jax.random.uniform(streams_of[13], (BLOCKS, HEADS), jnp.float32, -1.0, 4.0), -1.0, 4.0)
    forget_slope = jnp.clip(jax.random.uniform(streams_of[14], (BLOCKS, HEADS), jnp.float32, -3.0, 3.0), -3.0, 3.0)
    head_gain = jnp.clip(1.0 + 0.18 * jax.random.normal(streams_of[15], (BLOCKS, D), jnp.float32), 0.099609375, 1.8984375).astype(jnp.bfloat16)
    output_weight = scatter_about(streams_of[16], (BLOCKS, D, D), D ** -0.5, 0.125, ((2, 16),))
    return dict(tokens=tokens, lengths=lengths, cell_memory=cell_memory, key_sums=key_sums, stabilizer=stabilizer, norm_gain=norm_gain, query_weight=query_weight, key_weight=key_weight, value_weight=value_weight, outgate_weight=outgate_weight, ingate_weight=ingate_weight, forget_weight=forget_weight, ingate_bias=ingate_bias, forget_bias=forget_bias, forget_slope=forget_slope, head_gain=head_gain, output_weight=output_weight)


EPS = 1e-05

def one_block(tokens, position, memory, key_sums, stabilizer, norm_gain, query_weight, key_weight, value_weight, outgate_weight, ingate_weight, forget_weight, ingate_bias, forget_bias, forget_slope, head_gain, output_weight):
    batch_rows = tokens.shape[0]
    model_width = tokens.shape[1]
    head_count = stabilizer.shape[1]
    head_size = model_width // head_count
    tok_float = tokens.astype(jnp.float32)
    normed = (tok_float * lax.rsqrt(lax.optimization_barrier(jnp.mean(tok_float * tok_float, axis=-1, keepdims=True)) + EPS) * norm_gain.astype(jnp.float32)).astype(jnp.bfloat16)
    queries = jnp.dot(normed, query_weight, preferred_element_type=jnp.float32).astype(jnp.bfloat16)
    key_rows = (jnp.dot(normed, key_weight, preferred_element_type=jnp.float32) * head_size ** (-0.5)).astype(jnp.bfloat16)
    values = jnp.dot(normed, value_weight, preferred_element_type=jnp.float32).astype(jnp.bfloat16)
    outgate = jnp.dot(normed, outgate_weight, preferred_element_type=jnp.float32).astype(jnp.bfloat16)
    ingate = jnp.dot(normed, ingate_weight, preferred_element_type=jnp.float32) + ingate_bias
    forget = jax.nn.log_sigmoid(jnp.dot(normed, forget_weight, preferred_element_type=jnp.float32) + forget_bias + forget_slope * position[:, None])
    stab_new = jnp.maximum(forget + stabilizer, ingate)
    decays = jnp.exp(forget + stabilizer - stab_new)
    in_weight = jnp.exp(ingate - stab_new)
    query_heads = queries.astype(jnp.float32).reshape(batch_rows, head_count, head_size)
    key_heads = key_rows.astype(jnp.float32).reshape(batch_rows, head_count, head_size)
    value_heads = values.astype(jnp.float32).reshape(batch_rows, head_count, head_size)
    old_memory = memory.reshape(batch_rows, head_count, head_size, head_size)
    mem_new = decays[:, :, None, None] * old_memory + in_weight[:, :, None, None] * value_heads[:, :, :, None] * key_heads[:, :, None, :]
    sums_new = decays[:, :, None] * key_sums.reshape(batch_rows, head_count, head_size) + in_weight[:, :, None] * key_heads
    numerator = jnp.einsum('bhvk,bhk->bhv', mem_new, query_heads, precision=lax.Precision.HIGHEST)
    denominator = jnp.maximum(jnp.abs(lax.optimization_barrier(jnp.sum(sums_new * query_heads, axis=-1))), 1.0)
    hidden = numerator / denominator[:, :, None]
    gated_out = (hidden.reshape(batch_rows, model_width) * head_gain.astype(jnp.float32) * jax.nn.sigmoid(outgate.astype(jnp.float32))).astype(jnp.bfloat16)
    new_tokens = (tok_float + jnp.dot(gated_out, output_weight, preferred_element_type=jnp.float32)).astype(jnp.bfloat16)
    return (new_tokens, mem_new.reshape(batch_rows, model_width, head_size), sums_new.reshape(batch_rows, model_width), stab_new)

def reference(tokens, lengths, cell_memory, key_sums, stabilizer, norm_gain, query_weight, key_weight, value_weight, outgate_weight, ingate_weight, forget_weight, ingate_bias, forget_bias, forget_slope, head_gain, output_weight):
    position = lengths.astype(jnp.float32) / MAXLEN
    current = tokens
    memories, sums_list, stabs = ([], [], [])
    for block_id in range(BLOCKS):
        current, mem_new, sums_new, stab_new = one_block(current, position, cell_memory[block_id], key_sums[block_id], stabilizer[block_id], norm_gain[block_id], query_weight[block_id], key_weight[block_id], value_weight[block_id], outgate_weight[block_id], ingate_weight[block_id], forget_weight[block_id], ingate_bias[block_id], forget_bias[block_id], forget_slope[block_id], head_gain[block_id], output_weight[block_id])
        memories.append(mem_new)
        sums_list.append(sums_new)
        stabs.append(stab_new)
    return (current, jnp.stack(memories), jnp.stack(sums_list), jnp.stack(stabs))
```

```python
import functools

import jax
import jax.numpy as jnp
from jax import lax
from jax.experimental import pallas as pl
from jax.experimental.pallas import tpu as pltpu
from jax.sharding import PartitionSpec as P


MAXLEN = 4096
EPS = 1e-05
MIB = 1 << 20
PARTS = 3


VM = pl.BlockSpec(memory_space=pltpu.VMEM)
SM = pl.BlockSpec(memory_space=pltpu.SMEM)
HBM = pl.BlockSpec(memory_space=pltpu.HBM)
F32 = jnp.float32
BF16 = jnp.bfloat16


def gather_phases(count):
    bits = [1 << i for i in range(count.bit_length() - 1)][::-1]
    if len(bits) < 2:
        return [tuple(bits)] if bits else []
    low = bits[-1]
    rounds = [(bits[0] | low,)] if len(bits) > 1 else []
    middle = bits[1:-1]
    for at in range(0, len(middle), 2):
        pair = middle[at : at + 2]
        if len(pair) == 2:
            rounds.append((pair[0] | pair[1], pair[1] | low, pair[0] | low))
        else:
            rounds.append((pair[0] | low,))
    return rounds + [(low,)]


def swap(value, mask):
    return lax.ppermute(value, "tp", [(s, s ^ mask) for s in range(lax.axis_size("tp"))])


def gather(value):
    *rounds, last = gather_phases(lax.axis_size("tp"))
    blocks, masks = value[None], [0]
    for group in rounds:
        parts, held = [blocks], list(masks)
        for mask in group:
            parts.append(swap(blocks, mask))
            masks = masks + [m ^ mask for m in held]
        blocks = jnp.concatenate(parts, axis=0)
    far = swap(blocks, last[0])
    return blocks, far, masks, last[0]


def shares(steps):
    sizes = [steps // PARTS + (i < steps % PARTS) for i in range(PARTS)]
    return sizes[1:2] + sizes[0:1] + sizes[2:]


def call(kernel, out_shape, in_specs, out_specs, scratch=(), aliases=None, limit=4, flops=1 << 20):
    return pl.pallas_call(
        kernel,
        out_shape=out_shape,
        in_specs=in_specs,
        out_specs=out_specs,
        scratch_shapes=scratch,
        input_output_aliases=aliases or {},
        compiler_params=pltpu.CompilerParams(vmem_limit_bytes=limit * MIB),
        cost_estimate=pl.CostEstimate(flops=flops, bytes_accessed=1 << 20, transcendentals=0),
    )


def place(own, near, far, rows, masks, low):
    for j, mask in enumerate(masks):
        rows[own ^ mask] = near[j]
        rows[own ^ mask ^ low] = far[j]


def joined(rows):
    return jnp.concatenate([rows[i] for i in range(rows.shape[0])], axis=1)


def dot(a, b):
    return jnp.dot(a, b, preferred_element_type=F32)


def heads_kernel(layer, masks, low, scale, ids, near, far, gain, wq, wk, pair, normed, rows):
    place(ids[0], near, far, rows, masks, low)
    x = joined(rows).astype(F32)
    inv = lax.rsqrt(jnp.mean(x * x, axis=1, keepdims=True) + EPS)
    n = (x * inv * gain[layer : layer + 1].astype(F32)).astype(BF16)
    normed[...] = n
    width = wq.shape[2]
    both = dot(n, jnp.concatenate([wq[layer], wk[layer]], axis=1))
    pair[0] = both[:, :width].astype(BF16)
    pair[1] = (both[:, width:] * scale).astype(BF16)


def as_column(row):
    n = row.shape[1]
    same = lax.broadcasted_iota(jnp.int32, (n, n), 0) == lax.broadcasted_iota(jnp.int32, (n, n), 1)
    return jnp.sum(jnp.where(same, row, 0.0), axis=1, keepdims=True)


def gates_kernel(
    layer, ids, normed, wv, wo, wi, wf, ibias, fbias, slope, lengths, stab, old,
    values, outgate, factors, stab_new, columns, decays,
):
    n = normed[...]
    width = wv.shape[2]
    both = dot(n, jnp.concatenate([wv[layer], wo[layer]], axis=1))
    values[...] = both[:, :width].astype(BF16)
    outgate[...] = both[:, width:].astype(BF16)

    def logits(w):
        return lax.dot_general(w[layer], n, (((1,), (1,)), ((), ())), preferred_element_type=F32)

    row = slice(layer, layer + 1)
    position = lengths[...].astype(F32) / MAXLEN
    ingate = logits(wi) + as_column(ibias[row])
    forget = jax.nn.log_sigmoid(logits(wf) + as_column(fbias[row]) + as_column(slope[row]) * position)
    held = forget + stab[layer]
    top = jnp.maximum(held, ingate)
    for other in range(layer):
        stab_new[other] = old[other]
    stab_new[layer] = top
    index = lax.broadcasted_iota(jnp.int32, top.shape, 0)
    mine = index == ids[1]
    decay = jnp.sum(jnp.where(mine, jnp.exp(held - top), 0.0), axis=0, keepdims=True)
    weight = jnp.sum(jnp.where(mine, jnp.exp(ingate - top), 0.0), axis=0, keepdims=True)
    factors[...] = jnp.where(index == 0, decay, weight).T
    batch, lanes = n.shape[0], columns.shape[1]
    v = both[:, :width].astype(BF16).astype(F32) * factors[:, 1:2]
    if lanes > batch:
        v = jnp.concatenate([v, jnp.zeros((lanes - batch, width), F32)], axis=0)
    columns[...] = v.T.astype(BF16)
    decays[...] = jnp.broadcast_to(factors[:, 0:1], decays.shape)


def read_kernel(
    layer,
    rows,
    memory,
    head_pair,
    pair,
    values,
    outgate,
    factors,
    all_sums,
    sums,
    gain,
    old,
    gated,
    sums_new,
    kept,
    query,
    arrived,
):
    batch, width, _ = kept.shape
    chunks = batch // rows

    def fetch(i):
        part = pl.ds(i * rows, rows)
        return pltpu.make_async_copy(memory.at[layer, part], kept.at[part], arrived.at[i])

    for i in range(chunks):
        fetch(i).start()
    q = head_pair[0].astype(F32)
    query[...] = q
    lanes = -(-batch // 128) * 128
    lane = lax.broadcasted_iota(jnp.int32, (width, lanes), 1)
    total = jnp.zeros((width, lanes), F32)

    def some(i, total):
        fetch(i).wait()
        for r in range(rows):
            b = i * rows + r
            product = kept[b] * query[pl.ds(b, 1), :]
            column = jnp.sum(product, axis=1, keepdims=True)
            total = jnp.where(lane == b, column, total)
        return total

    read = lax.fori_loop(0, chunks, some, total).T[:batch]
    decay, weight = factors[:, 0:1], factors[:, 1:2]
    match = weight * jnp.sum(head_pair[1].astype(F32) * q, axis=1, keepdims=True)
    v = values[...].astype(F32)
    numerator = decay * read + match * v
    below = decay * jnp.sum(all_sums[layer] * q, axis=1, keepdims=True) + match
    hidden = numerator / jnp.maximum(jnp.abs(below), 1.0)
    gate = jax.nn.sigmoid(outgate[...].astype(F32))
    gated[...] = (hidden * gain[layer : layer + 1].astype(F32) * gate).astype(BF16)
    for other in range(layer):
        sums_new[other] = old[other]
    sums_new[layer] = decay * sums[layer] + weight * pair[1].astype(F32)


def out_kernel(layer, masks, low, ids, near, far, current, wo, after, rows):
    place(ids[0], near, far, rows, masks, low)
    total = current[...].astype(F32) + dot(joined(rows), wo[layer])
    after[...] = total.astype(BF16)


def update_kernel(first, rows, kept, columns, decays, head_pair, _old, new):
    batch, width, depth = kept.shape
    lanes = columns.shape[1]
    keys = head_pair[1]
    if lanes > batch:
        keys = jnp.concatenate([keys, jnp.zeros((lanes - batch, depth), BF16)], axis=0)
    lane = lax.broadcasted_iota(jnp.int32, columns.shape, 1)
    at = first + pl.program_id(0) * rows
    all_columns = columns[...]
    chosen = [jnp.where(lane == at + r, all_columns, jnp.zeros_like(all_columns)) for r in range(rows)]
    outer = dot(jnp.concatenate(chosen, axis=0), keys)
    for r in range(rows):
        new[0, r] = decays[pl.ds(at + r, 1), :] * kept[at + r] + outer[r * width : (r + 1) * width]


def in_hbm(x):
    return pltpu.with_memory_space_constraint(x, pltpu.HBM)


def load_kernel(count, *refs):
    arrived = refs[-1]
    copies = [pltpu.make_async_copy(refs[i], refs[count + i], arrived.at[i]) for i in range(count)]
    for copy in copies:
        copy.start()
    for copy in copies:
        copy.wait()


def load(*arrays):
    return pl.pallas_call(
        functools.partial(load_kernel, len(arrays)),
        out_shape=tuple(pltpu.VMEM(a.shape, a.dtype) for a in arrays),
        in_specs=[HBM] * len(arrays),
        out_specs=(VM,) * len(arrays),
        scratch_shapes=[pltpu.SemaphoreType.DMA((len(arrays),))],
        compiler_params=pltpu.CompilerParams(vmem_limit_bytes=MIB),
        cost_estimate=pl.CostEstimate(flops=1 << 20, bytes_accessed=1 << 20, transcendentals=0),
    )(*(in_hbm(a) for a in arrays))


def body(
    tokens,
    lengths,
    cell_memory,
    key_sums,
    stabilizer,
    norm_gain,
    query_weight,
    key_weight,
    value_weight,
    outgate_weight,
    ingate_weight,
    forget_weight,
    ingate_bias,
    forget_bias,
    forget_slope,
    head_gain,
    output_weight,
):
    count = lax.axis_size("tp")
    blocks, batch, width, depth = cell_memory.shape
    heads = stabilizer.shape[2]
    split_count = count // heads
    own = lax.axis_index("tp")
    ids = jnp.stack([own, own // split_count]).astype(jnp.int32)

    def whole_head(value):
        axis = value.ndim - 1
        for level in range(split_count.bit_length() - 1):
            partner = swap(value, 1 << level)
            upper = own // (1 << level) % 2 == 1
            value = jnp.concatenate(
                (jnp.where(upper, partner, value), jnp.where(upper, value, partner)), axis=axis
            )
        return value

    near, far, masks, low = gather(tokens)
    (sums, wq, wk, wv, wg, wo, wi, wf, ibias, fbias, slope, at, stab, norm_gain, head_gain, current) = load(
        key_sums,
        query_weight,
        key_weight,
        value_weight,
        outgate_weight,
        output_weight,
        jnp.swapaxes(ingate_weight, 1, 2),
        jnp.swapaxes(forget_weight, 1, 2),
        ingate_bias,
        forget_bias,
        forget_slope,
        lengths[None],
        jnp.swapaxes(stabilizer, 1, 2),
        norm_gain,
        head_gain,
        tokens,
    )
    all_sums = whole_head(sums)
    shape = jax.ShapeDtypeStruct
    rows = 8 if batch % 8 == 0 else 1
    lanes = -(-batch // 128) * 128
    new_memory, new_sums, new_stab = ids, sums, stab
    for layer in range(blocks):
        if layer:
            near, far, masks, low = gather(current)
        pair, normed = call(
            functools.partial(heads_kernel, layer, masks, low, depth ** (-0.5)),
            (shape((2, batch, width), BF16), pltpu.VMEM((batch, count * width), BF16)),
            [SM] + [VM] * 5,
            (VM, VM),
            [pltpu.VMEM((count, batch, width), BF16)],
        )(ids, near, far, norm_gain, wq, wk)
        head_pair = whole_head(pair)
        values, outgate, factors, new_stab, columns, decays = call(
            functools.partial(gates_kernel, layer),
            (
                shape((batch, width), BF16),
                shape((batch, width), BF16),
                shape((batch, heads), F32),
                shape(stab.shape, F32),
                pltpu.VMEM((width, lanes), BF16),
                pltpu.VMEM((batch, depth), F32),
            ),
            [SM] + [VM] * 11,
            (VM,) * 6,
        )(ids, normed, wv, wg, wi, wf, ibias, fbias, slope, at, stab, new_stab)
        gated, new_sums, kept = call(
            functools.partial(read_kernel, layer, rows),
            (
                shape((batch, width), BF16),
                shape(sums.shape, F32),
                pltpu.VMEM((batch, width, depth), F32),
            ),
            [HBM] + [VM] * 9,
            (VM, VM, VM),
            [pltpu.VMEM((batch, depth), F32), pltpu.SemaphoreType.DMA((batch // rows,))],
        )(in_hbm(cell_memory), head_pair, pair, values, outgate, factors, all_sums, sums, head_gain, new_sums)

        near, far, masks, low = gather(gated)
        first = 0
        for part, size in enumerate(shares(batch // rows)):
            if not size:
                continue
            new_memory = pl.pallas_call(
                functools.partial(update_kernel, first * rows, rows),
                out_shape=shape(cell_memory.shape, F32),
                grid=(size,),
                in_specs=[VM] * 4 + [pl.BlockSpec(memory_space=pl.ANY)],
                out_specs=pl.BlockSpec(
                    (1, rows, width, depth),
                    lambda i, layer=layer, first=first: (layer, first + i, 0, 0),
                ),
                input_output_aliases={} if layer == part == 0 else {4: 0},
                compiler_params=pltpu.CompilerParams(vmem_limit_bytes=8 * MIB),
                cost_estimate=pl.CostEstimate(flops=1 << 22, bytes_accessed=1 << 20, transcendentals=0),
            )(kept, columns, decays, head_pair, new_memory)
            first += size

        current = call(
            functools.partial(out_kernel, layer, masks, low),
            shape((batch, width), BF16),
            [SM] + [VM] * 4,
            VM,
            [pltpu.VMEM((count, batch, width), BF16)],
        )(ids, near, far, current, wo)
    return current, new_memory, new_sums, jnp.swapaxes(new_stab, 1, 2)


def solution(mesh):
    in_specs = (
        P("grp", "tp"),
        P("grp"),
        P(None, "grp", "tp", None),
        P(None, "grp", "tp"),
        P(None, "grp", None),
        P(),
        P(None, None, "tp"),
        P(None, None, "tp"),
        P(None, None, "tp"),
        P(None, None, "tp"),
        P(),
        P(),
        P(),
        P(),
        P(),
        P(None, "tp"),
        P(None, None, "tp"),
    )
    out_specs = (
        P("grp", "tp"),
        P(None, "grp", "tp", None),
        P(None, "grp", "tp"),
        P(None, "grp", None),
    )

    return jax.shard_map(body, mesh=mesh, in_specs=in_specs, out_specs=out_specs, check_vma=False)
```

```python
import functools

import jax
import jax.numpy as jnp
from jax import lax
from jax.experimental import pallas as pl
from jax.experimental.pallas import tpu as pltpu
from jax.sharding import PartitionSpec as P


MAXLEN = 4096
EPS = 1e-05
MIB = 1 << 20
BYTES = 1 << 26


VM = pl.BlockSpec(memory_space=pltpu.VMEM)
SM = pl.BlockSpec(memory_space=pltpu.SMEM)
HBM = pl.BlockSpec(memory_space=pltpu.HBM)
F32 = jnp.float32
BF16 = jnp.bfloat16


def gather_phases(count):
    bits = [1 << i for i in range(count.bit_length() - 1)][::-1]
    if len(bits) < 2:
        return [tuple(bits)] if bits else []
    low = bits[-1]
    rounds = [(bits[0] | low,)] if len(bits) > 1 else []
    middle = bits[1:-1]
    for at in range(0, len(middle), 2):
        pair = middle[at : at + 2]
        if len(pair) == 2:
            rounds.append((pair[0] | pair[1], pair[1] | low, pair[0] | low))
        else:
            rounds.append((pair[0] | low,))
    return rounds + [(low,)]


def swap(value, mask):
    return lax.ppermute(value, "tp", [(s, s ^ mask) for s in range(lax.axis_size("tp"))])


def gather(value, held):
    *rounds, last = gather_phases(lax.axis_size("tp"))
    blocks, masks = value[None], [0]
    first = held[None]
    for number, group in enumerate(rounds):
        parts, before = [first if number == 0 else blocks], list(masks)
        for mask in group:
            parts.append(swap(blocks, mask))
            masks = masks + [m ^ mask for m in before]
        blocks = jnp.concatenate(parts, axis=0)
    far = swap(blocks, last[0])
    return blocks, far, masks, last[0]


def call(kernel, out_shape, in_specs, out_specs, scratch=(), aliases=None, limit=4, flops=1 << 20):
    return pl.pallas_call(
        kernel,
        out_shape=out_shape,
        in_specs=in_specs,
        out_specs=out_specs,
        scratch_shapes=scratch,
        input_output_aliases=aliases or {},
        compiler_params=pltpu.CompilerParams(vmem_limit_bytes=limit * MIB),
        cost_estimate=pl.CostEstimate(flops=flops, bytes_accessed=BYTES, transcendentals=0),
    )


def place(near, far, rows, masks, low):
    own = lax.axis_index("tp")
    for j, mask in enumerate(masks):
        rows[own ^ mask] = near[j]
        rows[own ^ mask ^ low] = far[j]


def joined(rows):
    return jnp.concatenate([rows[i] for i in range(rows.shape[0])], axis=1)


def dot(a, b):
    return jnp.dot(a, b, preferred_element_type=F32)


def heads_kernel(layer, masks, low, scale, near, far, gain, wq, wk, pair, normed, rows):
    place(near, far, rows, masks, low)
    x = joined(rows).astype(F32)
    inv = lax.rsqrt(jnp.mean(x * x, axis=1, keepdims=True) + EPS)
    n = (x * inv * gain[layer : layer + 1].astype(F32)).astype(BF16)
    normed[...] = n
    width = wq.shape[1]
    both = dot(n, jnp.concatenate([wq[...], wk[...]], axis=1))
    pair[0] = both[:, :width].astype(BF16)
    pair[1] = (both[:, width:] * scale).astype(BF16)


def as_column(row):
    n = row.shape[1]
    same = lax.broadcasted_iota(jnp.int32, (n, n), 0) == lax.broadcasted_iota(jnp.int32, (n, n), 1)
    return jnp.sum(jnp.where(same, row, 0.0), axis=1, keepdims=True)


def gates_kernel(
    layer, split, normed, wv, wo, wi, wf, ibias, fbias, slope, lengths, stab, old,
    values, outgate, factors, stab_new, columns, decays,
):
    n = normed[...]
    width = wv.shape[1]
    both = dot(n, jnp.concatenate([wv[...], wo[...]], axis=1))
    values[...] = both[:, :width].astype(BF16)
    outgate[...] = both[:, width:].astype(BF16)

    def logits(w):
        return lax.dot_general(w[layer], n, (((1,), (1,)), ((), ())), preferred_element_type=F32)

    row = slice(layer, layer + 1)
    position = lengths[...].astype(F32) / MAXLEN
    ingate = logits(wi) + as_column(ibias[row])
    forget = jax.nn.log_sigmoid(logits(wf) + as_column(fbias[row]) + as_column(slope[row]) * position)
    held = forget + stab[layer]
    top = jnp.maximum(held, ingate)
    for other in range(layer):
        stab_new[other] = old[other]
    stab_new[layer] = top
    index = lax.broadcasted_iota(jnp.int32, top.shape, 0)
    mine = index == lax.axis_index("tp") // split
    decay = jnp.sum(jnp.where(mine, jnp.exp(held - top), 0.0), axis=0, keepdims=True)
    weight = jnp.sum(jnp.where(mine, jnp.exp(ingate - top), 0.0), axis=0, keepdims=True)
    factors[...] = jnp.where(index == 0, decay, weight).T
    batch, lanes = n.shape[0], columns.shape[1]
    v = both[:, :width].astype(BF16).astype(F32) * factors[:, 1:2]
    if lanes > batch:
        v = jnp.concatenate([v, jnp.zeros((lanes - batch, width), F32)], axis=0)
    columns[...] = v.T
    decays[...] = jnp.broadcast_to(factors[:, 0:1], decays.shape)


def in_order(parts, rows):
    local = lax.rem(lax.axis_index("tp"), len(parts))
    for mask, part in enumerate(parts):
        rows[local ^ mask] = part[...]


def read_kernel(layer, split, rows, memory, kept, *refs):
    pairs, refs = refs[:split], refs[split:]
    sums, refs = refs[:split], refs[split:]
    values, outgate, factors, gain, old, gated, sums_new, keys, rest, query, pieces, arrived = refs
    (first, width, depth), batch = kept.shape, values.shape[0]
    lanes = -(-batch // 128) * 128

    def fetch(i):
        part = pl.ds(i * rows, rows)
        return pltpu.make_async_copy(memory.at[layer, pl.ds(first + i * rows, rows)], rest.at[part], arrived.at[i])

    for i in range((batch - first) // rows):
        fetch(i).start()
    in_order(pairs, pieces)
    q = jnp.concatenate([pieces[i, 0] for i in range(split)], axis=1).astype(F32)
    query[...] = q
    key = jnp.concatenate([pieces[i, 1] for i in range(split)], axis=1).astype(F32)
    keys[...] = key
    lane = lax.broadcasted_iota(jnp.int32, (width, lanes), 1)

    def add(state, i, at, total):
        for r in range(rows):
            b = at + i * rows + r
            product = state[i * rows + r] * query[pl.ds(b, 1), :]
            column = jnp.sum(product, axis=1, keepdims=True)
            total = jnp.where(lane == b, column, total)
        return total

    def late(i, total):
        fetch(i).wait()
        return add(rest, i, first, total)

    total = jnp.zeros((width, lanes), F32)
    total = lax.fori_loop(0, first // rows, lambda i, total: add(kept, i, 0, total), total)
    total = lax.fori_loop(0, (batch - first) // rows, late, total)
    read = total.T[:batch]
    decay, weight = factors[:, 0:1], factors[:, 1:2]
    match = weight * jnp.sum(key * q, axis=1, keepdims=True)
    v = values[...].astype(F32)
    numerator = decay * read + match * v
    held = sum(s[layer] * p[0].astype(F32) for s, p in zip(sums, pairs))
    below = decay * jnp.sum(held, axis=1, keepdims=True) + match
    hidden = numerator / jnp.maximum(jnp.abs(below), 1.0)
    gate = jax.nn.sigmoid(outgate[...].astype(F32))
    gated[...] = (hidden * gain[layer : layer + 1].astype(F32) * gate).astype(BF16)
    for other in range(layer):
        sums_new[other] = old[other]
    sums_new[layer] = decay * sums[0][layer] + weight * pairs[0][1].astype(F32)


def out_kernel(masks, low, near, far, current, wo, after, rows):
    place(near, far, rows, masks, low)
    total = current[...].astype(F32) + dot(joined(rows), wo[...])
    after[...] = total.astype(BF16)


def update_kernel(layer, first, rows, kept, columns, decays, keys, _old, new, staged, sent):
    batch, width, depth = kept.shape
    lanes = columns.shape[1]

    def send(i):
        part = pl.ds(i * rows, rows)
        return pltpu.make_async_copy(staged.at[part], new.at[layer, pl.ds(first + i * rows, rows)], sent.at[i])

    def some(i, carry):
        at = first + i * rows
        turned = pltpu.roll(columns[...], lanes - at, axis=1)
        for r in range(rows):
            column = jnp.broadcast_to(turned[:, r : r + 1], (width, depth))
            key = keys[pl.ds(at + r, 1), :]
            staged[i * rows + r] = decays[pl.ds(at + r, 1), :] * kept[i * rows + r] + column * key
        send(i).start()
        return carry

    lax.fori_loop(0, batch // rows, some, 0)
    for i in range(batch // rows):
        send(i).wait()


def in_hbm(x):
    return pltpu.with_memory_space_constraint(x, pltpu.HBM)


def load_kernel(layer, whole, sliced, *refs):
    arrived, count = refs[-1], whole + sliced
    copies = []
    for i in range(count):
        source = refs[i] if i < whole else refs[i].at[layer]
        copies.append(pltpu.make_async_copy(source, refs[count + i], arrived.at[i]))
    for copy in copies:
        copy.start()
    for copy in copies:
        copy.wait()


def load(layer, whole, sliced):
    count = len(whole) + len(sliced)
    shapes = [a.shape for a in whole] + [a.shape[1:] for a in sliced]
    return call(
        functools.partial(load_kernel, layer, len(whole), len(sliced)),
        tuple(pltpu.VMEM(s, a.dtype) for s, a in zip(shapes, (*whole, *sliced))),
        [HBM] * count,
        (VM,) * count,
        [pltpu.SemaphoreType.DMA((count,))],
    )(*(in_hbm(a) for a in (*whole, *sliced)))


def state_kernel(layer, rows, memory, kept, arrived):
    copies = []
    for i in range(kept.shape[0] // rows):
        part = pl.ds(i * rows, rows)
        copies.append(pltpu.make_async_copy(memory.at[layer, part], kept.at[part], arrived.at[i]))
    for copy in copies:
        copy.start()
    for copy in copies:
        copy.wait()


def body(
    tokens,
    lengths,
    cell_memory,
    key_sums,
    stabilizer,
    norm_gain,
    query_weight,
    key_weight,
    value_weight,
    outgate_weight,
    ingate_weight,
    forget_weight,
    ingate_bias,
    forget_bias,
    forget_slope,
    head_gain,
    output_weight,
):
    count = lax.axis_size("tp")
    blocks, batch, width, depth = cell_memory.shape
    heads = stabilizer.shape[2]
    split = count // heads

    def pieces(value):
        found = [value]
        for mask in range(1, split):
            found.append(swap(value, mask))
        return found

    shape = jax.ShapeDtypeStruct
    rows = 8 if batch % 8 == 0 else 1
    lanes = -(-batch // 128) * 128
    first = batch // rows // 2 * rows
    sizes = (first, batch - first)
    weights = [query_weight, key_weight, value_weight, outgate_weight, output_weight]
    own_sums, wi, wf, ibias, fbias, slope, at, stab, norm_gain, head_gain, current, *loaded = load(
        0,
        [
            key_sums,
            jnp.swapaxes(ingate_weight, 1, 2),
            jnp.swapaxes(forget_weight, 1, 2),
            ingate_bias,
            forget_bias,
            forget_slope,
            lengths[None],
            jnp.swapaxes(stabilizer, 1, 2),
            norm_gain,
            head_gain,
            tokens,
        ],
        weights,
    )
    near, far, masks, low = gather(tokens, current)
    sums = pieces(own_sums)
    memory = in_hbm(cell_memory)
    new_memory, new_sums, new_stab = at, own_sums, stab
    for layer in range(blocks):
        if layer:
            near, far, masks, low = gather(current, current)
            loaded = load(layer, [], weights)
        wq, wk, wv, wg, wo = loaded
        kept = call(
            functools.partial(state_kernel, layer, rows),
            pltpu.VMEM((first, width, depth), F32),
            [HBM],
            VM,
            [pltpu.SemaphoreType.DMA((first // rows,))],
        )(memory)
        pair, normed = call(
            functools.partial(heads_kernel, layer, masks, low, depth ** (-0.5)),
            (shape((2, batch, width), BF16), pltpu.VMEM((batch, count * width), BF16)),
            [VM] * 5,
            (VM, VM),
            [pltpu.VMEM((count, batch, width), BF16)],
        )(near, far, norm_gain, wq, wk)
        pairs = pieces(pair)
        values, outgate, factors, new_stab, columns, decays = call(
            functools.partial(gates_kernel, layer, split),
            (
                shape((batch, width), BF16),
                shape((batch, width), BF16),
                shape((batch, heads), F32),
                shape(stab.shape, F32),
                pltpu.VMEM((width, lanes), F32),
                pltpu.VMEM((batch, depth), F32),
            ),
            [VM] * 11,
            (VM,) * 6,
        )(normed, wv, wg, wi, wf, ibias, fbias, slope, at, stab, new_stab)
        gated, new_sums, keys, rest = call(
            functools.partial(read_kernel, layer, split, rows),
            (
                shape((batch, width), BF16),
                shape(own_sums.shape, F32),
                pltpu.VMEM((batch, depth), F32),
                pltpu.VMEM((batch - first, width, depth), F32),
            ),
            [HBM] + [VM] * (6 + 2 * split),
            (VM,) * 4,
            [
                pltpu.VMEM((batch, depth), F32),
                pltpu.VMEM((split, 2, batch, width), BF16),
                pltpu.SemaphoreType.DMA(((batch - first) // rows,)),
            ],
        )(memory, kept, *pairs, *sums, values, outgate, factors, head_gain, new_sums)

        near, far, masks, low = gather(gated, gated)
        for part, state in enumerate((kept, rest)):
            new_memory = call(
                functools.partial(update_kernel, layer, part * first, rows),
                shape(cell_memory.shape, F32),
                [VM] * 4 + [HBM],
                HBM,
                [
                    pltpu.VMEM((sizes[part], width, depth), F32),
                    pltpu.SemaphoreType.DMA((sizes[part] // rows,)),
                ],
                {} if layer == part == 0 else {4: 0},
                limit=8,
            )(state, columns, decays, keys, in_hbm(new_memory))

        current = call(
            functools.partial(out_kernel, masks, low),
            shape((batch, width), BF16),
            [VM] * 4,
            VM,
            [pltpu.VMEM((count, batch, width), BF16)],
        )(near, far, current, wo)
    return current, new_memory, new_sums, jnp.swapaxes(new_stab, 1, 2)


def solution(mesh):
    in_specs = (
        P("grp", "tp"),
        P("grp"),
        P(None, "grp", "tp", None),
        P(None, "grp", "tp"),
        P(None, "grp", None),
        P(),
        P(None, None, "tp"),
        P(None, None, "tp"),
        P(None, None, "tp"),
        P(None, None, "tp"),
        P(),
        P(),
        P(),
        P(),
        P(),
        P(None, "tp"),
        P(None, None, "tp"),
    )
    out_specs = (
        P("grp", "tp"),
        P(None, "grp", "tp", None),
        P(None, "grp", "tp"),
        P(None, "grp", None),
    )

    return jax.shard_map(body, mesh=mesh, in_specs=in_specs, out_specs=out_specs, check_vma=False)
```

```python
import functools

import jax
import jax.numpy as jnp
from jax import lax
from jax.experimental import pallas as pl
from jax.experimental.pallas import tpu as pltpu
from jax.sharding import PartitionSpec as P


MAXLEN = 4096
EPS = 1e-05
MIB = 1 << 20
LANES = 128
EARLY = (6, 5)
DIRECT = 4
BYTES = 1 << 26


VM = pl.BlockSpec(memory_space=pltpu.VMEM)
SM = pl.BlockSpec(memory_space=pltpu.SMEM)
HBM = pl.BlockSpec(memory_space=pltpu.HBM)
F32 = jnp.float32
BF16 = jnp.bfloat16


def gather_phases(count):
    bits = [1 << i for i in range(count.bit_length() - 1)][::-1]
    if len(bits) < 2:
        return [tuple(bits)] if bits else []
    low = bits[-1]
    rounds = [(bits[0] | low,)] if len(bits) > 1 else []
    middle = bits[1:-1]
    for at in range(0, len(middle), 2):
        pair = middle[at : at + 2]
        if len(pair) == 2:
            rounds.append((pair[0] | pair[1] | low, pair[1] | low, pair[0] | low))
        else:
            rounds.append((pair[0] | low,))
    return rounds + [(low,)]


def swap(value, mask):
    return lax.ppermute(value, "tp", [(s, s ^ mask) for s in range(lax.axis_size("tp"))])


def gather(value, held):
    *rounds, last = gather_phases(lax.axis_size("tp"))
    blocks, masks = value[None], [0]
    first = held[None]
    for number, group in enumerate(rounds):
        parts, before = [first if number == 0 else blocks], list(masks)
        for mask in group:
            parts.append(swap(blocks, mask))
            masks = masks + [m ^ mask for m in before]
        blocks = jnp.concatenate(parts, axis=0)
    far = swap(blocks, last[0])
    return blocks, far, masks, last[0]


def call(kernel, out_shape, in_specs, out_specs, scratch=(), aliases=None, limit=4, flops=1 << 20):
    return pl.pallas_call(
        kernel,
        out_shape=out_shape,
        in_specs=in_specs,
        out_specs=out_specs,
        scratch_shapes=scratch,
        input_output_aliases=aliases or {},
        compiler_params=pltpu.CompilerParams(vmem_limit_bytes=limit * MIB),
        cost_estimate=pl.CostEstimate(flops=flops, bytes_accessed=BYTES, transcendentals=0),
    )


def place(near, far, rows, masks, low):
    own = lax.axis_index("tp")
    for j, mask in enumerate(masks):
        rows[own ^ mask] = near[j]
        rows[own ^ mask ^ low] = far[j]


def joined(rows):
    return jnp.concatenate([rows[i] for i in range(rows.shape[0])], axis=1)


def dot(a, b):
    return jnp.dot(a, b, preferred_element_type=F32)


def heads_kernel(layer, masks, low, scale, near, far, gain, wq, wk, pair, normed, rows):
    place(near, far, rows, masks, low)
    x = joined(rows).astype(F32)
    inv = lax.rsqrt(jnp.mean(x * x, axis=1, keepdims=True) + EPS)
    n = (x * inv * gain[layer : layer + 1].astype(F32)).astype(BF16)
    normed[...] = n
    width = wq.shape[1]
    both = dot(n, jnp.concatenate([wq[...], wk[...]], axis=1))
    pair[0] = both[:, :width].astype(BF16)
    pair[1] = (both[:, width:] * scale).astype(BF16)


def as_column(row):
    n = row.shape[1]
    same = lax.broadcasted_iota(jnp.int32, (n, n), 0) == lax.broadcasted_iota(jnp.int32, (n, n), 1)
    return jnp.sum(jnp.where(same, row, 0.0), axis=1, keepdims=True)


def gates_kernel(
    layer, split, normed, wv, wo, wi, wf, ibias, fbias, slope, lengths, stab,
    values, outgate, factors, stab_new, columns, decays,
):
    n = normed[...]
    width = wv.shape[1]
    both = dot(n, jnp.concatenate([wv[...], wo[...]], axis=1))
    values[...] = both[:, :width].astype(BF16)
    outgate[...] = both[:, width:].astype(BF16)

    def logits(w):
        return lax.dot_general(w[layer], n, (((1,), (1,)), ((), ())), preferred_element_type=F32)

    row = slice(layer, layer + 1)
    position = lengths[...].astype(F32) / MAXLEN
    ingate = logits(wi) + as_column(ibias[row])
    forget = jax.nn.log_sigmoid(logits(wf) + as_column(fbias[row]) + as_column(slope[row]) * position)
    held = forget + stab[layer]
    top = jnp.maximum(held, ingate)
    stab_new[...] = top
    index = lax.broadcasted_iota(jnp.int32, top.shape, 0)
    mine = index == lax.axis_index("tp") // split
    decay = jnp.sum(jnp.where(mine, jnp.exp(held - top), 0.0), axis=0, keepdims=True)
    weight = jnp.sum(jnp.where(mine, jnp.exp(ingate - top), 0.0), axis=0, keepdims=True)
    factors[...] = jnp.where(index == 0, decay, weight).T
    batch, lanes = n.shape[0], columns.shape[1]
    v = both[:, :width].astype(BF16).astype(F32) * factors[:, 1:2]
    if lanes > batch:
        v = jnp.concatenate([v, jnp.zeros((lanes - batch, width), F32)], axis=0)
    columns[...] = v.T
    decays[...] = jnp.broadcast_to(factors[:, 0:1], decays.shape)


def in_order(parts, rows):
    local = lax.rem(lax.axis_index("tp"), len(parts))
    for mask, part in enumerate(parts):
        rows[local ^ mask] = part[...]


def read_kernel(layer, split, rows, memory, kept, *refs):
    pairs, refs = refs[:split], refs[split:]
    sums, refs = refs[:split], refs[split:]
    values, outgate, factors, gain, gated, sums_new, keys, rest, query, pieces, arrived = refs
    (first, width, depth), batch = kept.shape, values.shape[0]
    lanes = -(-batch // LANES) * LANES

    def fetch(i):
        part = pl.ds(i * rows, rows)
        return pltpu.make_async_copy(memory.at[layer, pl.ds(first + i * rows, rows)], rest.at[part], arrived.at[i])

    for i in range((batch - first) // rows):
        fetch(i).start()
    in_order(pairs, pieces)
    q = jnp.concatenate([pieces[i, 0] for i in range(split)], axis=1).astype(F32)
    query[...] = q
    key = jnp.concatenate([pieces[i, 1] for i in range(split)], axis=1).astype(F32)
    keys[...] = key
    lane = lax.broadcasted_iota(jnp.int32, (width, lanes), 1)

    ones = jnp.ones((LANES, LANES), BF16)
    direct = rows * DIRECT // 8

    def add(state, i, at, total):
        products = []
        for r in range(rows):
            x = state[i * rows + r] * query[pl.ds(at + i * rows + r, 1), :]
            products.append(sum(x[:, j : j + LANES] for j in range(0, depth, LANES)))
        if direct < rows:
            summed = dot(jnp.concatenate(products[direct:], axis=0).astype(BF16), ones)
        for r in range(rows):
            if r < direct:
                column = jnp.sum(products[r], axis=1, keepdims=True)
            else:
                column = summed[(r - direct) * width : (r - direct + 1) * width]
            total = jnp.where(lane == at + i * rows + r, column, total)
        return total

    def late(i, total):
        fetch(i).wait()
        return add(rest, i, first, total)

    total = jnp.zeros((width, lanes), F32)
    total = lax.fori_loop(0, first // rows, lambda i, total: add(kept, i, 0, total), total)
    total = lax.fori_loop(0, (batch - first) // rows, late, total)
    read = total.T[:batch]
    decay, weight = factors[:, 0:1], factors[:, 1:2]
    match = weight * jnp.sum(key * q, axis=1, keepdims=True)
    v = values[...].astype(F32)
    numerator = decay * read + match * v
    held = sum(s[layer] * p[0].astype(F32) for s, p in zip(sums, pairs))
    below = decay * jnp.sum(held, axis=1, keepdims=True) + match
    hidden = numerator / jnp.maximum(jnp.abs(below), 1.0)
    gate = jax.nn.sigmoid(outgate[...].astype(F32))
    gated[...] = (hidden * gain[layer : layer + 1].astype(F32) * gate).astype(BF16)
    sums_new[...] = decay * sums[0][layer] + weight * pairs[0][1].astype(F32)


def out_kernel(masks, low, near, far, current, wo, after, rows):
    place(near, far, rows, masks, low)
    total = current[...].astype(F32) + dot(joined(rows), wo[...])
    after[...] = total.astype(BF16)


def update_kernel(layer, start, count, rows, kept, rest, columns, decays, keys, _old, new, staged, sent):
    first, width, depth = kept.shape
    lanes = columns.shape[1]

    def send(i):
        part = pl.ds(i * rows, rows)
        return pltpu.make_async_copy(staged.at[part], new.at[layer, pl.ds(start + i * rows, rows)], sent.at[i])

    lane = lax.broadcasted_iota(jnp.int32, columns.shape, 1)
    direct = rows * DIRECT // 8
    operand = keys[...].astype(BF16)
    if lanes > keys.shape[0]:
        operand = jnp.concatenate([operand, jnp.zeros((lanes - keys.shape[0], depth), BF16)], axis=0)

    def some(state, skipped, i, carry):
        at = start + i * rows
        if direct < rows:
            chosen = [jnp.where(lane == at + r, columns[...], 0.0).astype(BF16) for r in range(direct, rows)]
            outer = dot(jnp.concatenate(chosen, axis=0), operand)
        if direct:
            turned = pltpu.roll(columns[...], lanes - at, axis=1)
        for r in range(rows):
            if r < direct:
                added = jnp.broadcast_to(turned[:, r : r + 1], (width, depth)) * keys[pl.ds(at + r, 1), :]
            else:
                added = outer[(r - direct) * width : (r - direct + 1) * width]
            staged[i * rows + r] = decays[pl.ds(at + r, 1), :] * state[at - skipped + r] + added
        send(i).start()
        return carry

    steps = count // rows
    middle = min(max((first - start) // rows, 0), steps)
    lax.fori_loop(0, middle, functools.partial(some, kept, 0), 0)
    lax.fori_loop(middle, steps, functools.partial(some, rest, first), 0)
    for i in range(steps):
        send(i).wait()


def store_kernel(blocks, *refs):
    parts, (sums, stab, sent) = refs[: 2 * blocks], refs[2 * blocks :]
    copies = []
    for i, part in enumerate(parts):
        target = sums.at[i] if i < blocks else stab.at[i - blocks]
        copies.append(pltpu.make_async_copy(part, target, sent.at[i]))
    for copy in copies:
        copy.start()
    for copy in copies:
        copy.wait()


def in_hbm(x):
    return pltpu.with_memory_space_constraint(x, pltpu.HBM)


def load_kernel(layer, whole, sliced, *refs):
    arrived, count = refs[-1], whole + sliced
    copies = []
    for i in range(count):
        source = refs[i] if i < whole else refs[i].at[layer]
        copies.append(pltpu.make_async_copy(source, refs[count + i], arrived.at[i]))
    for copy in copies:
        copy.start()
    for copy in copies:
        copy.wait()


def load(layer, whole, sliced):
    count = len(whole) + len(sliced)
    shapes = [a.shape for a in whole] + [a.shape[1:] for a in sliced]
    return call(
        functools.partial(load_kernel, layer, len(whole), len(sliced)),
        tuple(pltpu.VMEM(s, a.dtype) for s, a in zip(shapes, (*whole, *sliced))),
        [HBM] * count,
        (VM,) * count,
        [pltpu.SemaphoreType.DMA((count,))],
    )(*(in_hbm(a) for a in (*whole, *sliced)))


def state_kernel(layer, rows, memory, kept, arrived):
    copies = []
    for i in range(kept.shape[0] // rows):
        part = pl.ds(i * rows, rows)
        copies.append(pltpu.make_async_copy(memory.at[layer, part], kept.at[part], arrived.at[i]))
    for copy in copies:
        copy.start()
    for copy in copies:
        copy.wait()


def body(
    tokens,
    lengths,
    cell_memory,
    key_sums,
    stabilizer,
    norm_gain,
    query_weight,
    key_weight,
    value_weight,
    outgate_weight,
    ingate_weight,
    forget_weight,
    ingate_bias,
    forget_bias,
    forget_slope,
    head_gain,
    output_weight,
):
    count = lax.axis_size("tp")
    blocks, batch, width, depth = cell_memory.shape
    heads = stabilizer.shape[2]
    split = count // heads

    def pieces(value):
        found = [value]
        for mask in range(1, split):
            found.append(swap(value, mask))
        return found

    shape = jax.ShapeDtypeStruct
    rows = 8 if batch % 8 == 0 else 1
    lanes = -(-batch // LANES) * LANES
    sizes = (batch // rows // 2 * rows, batch - batch // rows // 2 * rows)
    weights = [query_weight, key_weight, value_weight, outgate_weight, output_weight]
    own_sums, wi, wf, ibias, fbias, slope, at, stab, norm_gain, head_gain, current, *loaded = load(
        0,
        [
            key_sums,
            jnp.swapaxes(ingate_weight, 1, 2),
            jnp.swapaxes(forget_weight, 1, 2),
            ingate_bias,
            forget_bias,
            forget_slope,
            lengths[None],
            jnp.swapaxes(stabilizer, 1, 2),
            norm_gain,
            head_gain,
            tokens,
        ],
        weights,
    )
    near, far, masks, low = gather(tokens, current)
    sums = pieces(own_sums)
    memory = in_hbm(cell_memory)
    new_memory, sums_out, stabs = at, [], []
    for layer in range(blocks):
        if layer:
            near, far, masks, low = gather(current, current)
            loaded = load(layer, [], weights)
        wq, wk, wv, wg, wo = loaded
        first = batch // rows * EARLY[layer > 0] // 10 * rows
        kept = call(
            functools.partial(state_kernel, layer, rows),
            pltpu.VMEM((first, width, depth), F32),
            [HBM],
            VM,
            [pltpu.SemaphoreType.DMA((first // rows,))],
        )(memory)
        pair, normed = call(
            functools.partial(heads_kernel, layer, masks, low, depth ** (-0.5)),
            (shape((2, batch, width), BF16), pltpu.VMEM((batch, count * width), BF16)),
            [VM] * 5,
            (VM, VM),
            [pltpu.VMEM((count, batch, width), BF16)],
        )(near, far, norm_gain, wq, wk)
        pairs = pieces(pair)
        values, outgate, factors, new_stab, columns, decays = call(
            functools.partial(gates_kernel, layer, split),
            (
                shape((batch, width), BF16),
                shape((batch, width), BF16),
                shape((batch, heads), F32),
                pltpu.VMEM(stab.shape[1:], F32),
                pltpu.VMEM((width, lanes), F32),
                pltpu.VMEM((batch, depth), F32),
            ),
            [VM] * 10,
            (VM,) * 6,
        )(normed, wv, wg, wi, wf, ibias, fbias, slope, at, stab)
        stabs.append(new_stab)
        gated, new_sums, keys, rest = call(
            functools.partial(read_kernel, layer, split, rows),
            (
                shape((batch, width), BF16),
                pltpu.VMEM((batch, width), F32),
                pltpu.VMEM((batch, depth), F32),
                pltpu.VMEM((batch - first, width, depth), F32),
            ),
            [HBM] + [VM] * (5 + 2 * split),
            (VM,) * 4,
            [
                pltpu.VMEM((batch, depth), F32),
                pltpu.VMEM((split, 2, batch, width), BF16),
                pltpu.SemaphoreType.DMA(((batch - first) // rows,)),
            ],
        )(memory, kept, *pairs, *sums, values, outgate, factors, head_gain)
        sums_out.append(new_sums)

        near, far, masks, low = gather(gated, gated)
        for part, size in enumerate(sizes):
            new_memory = call(
                functools.partial(update_kernel, layer, part * sizes[0], size, rows),
                shape(cell_memory.shape, F32),
                [VM] * 5 + [HBM],
                HBM,
                [pltpu.VMEM((size, width, depth), F32), pltpu.SemaphoreType.DMA((size // rows,))],
                {} if layer == part == 0 else {5: 0},
                limit=8,
            )(kept, rest, columns, decays, keys, in_hbm(new_memory))

        current = call(
            functools.partial(out_kernel, masks, low),
            shape((batch, width), BF16),
            [VM] * 4,
            VM,
            [pltpu.VMEM((count, batch, width), BF16)],
        )(near, far, current, wo)
    new_sums, new_stab = call(
        functools.partial(store_kernel, blocks),
        (shape(own_sums.shape, F32), shape(stab.shape, F32)),
        [VM] * (2 * blocks),
        (HBM, HBM),
        [pltpu.SemaphoreType.DMA((2 * blocks,))],
    )(*sums_out, *stabs)
    return current, new_memory, new_sums, jnp.swapaxes(new_stab, 1, 2)


def solution(mesh):
    in_specs = (
        P("grp", "tp"),
        P("grp"),
        P(None, "grp", "tp", None),
        P(None, "grp", "tp"),
        P(None, "grp", None),
        P(),
        P(None, None, "tp"),
        P(None, None, "tp"),
        P(None, None, "tp"),
        P(None, None, "tp"),
        P(),
        P(),
        P(),
        P(),
        P(),
        P(None, "tp"),
        P(None, None, "tp"),
    )
    out_specs = (
        P("grp", "tp"),
        P(None, "grp", "tp", None),
        P(None, "grp", "tp"),
        P(None, "grp", None),
    )

    return jax.shard_map(body, mesh=mesh, in_specs=in_specs, out_specs=out_specs, check_vma=False)
```

```python
import functools

import jax
import jax.numpy as jnp
from jax import lax
from jax.experimental import pallas as pl
from jax.experimental.pallas import tpu as pltpu
from jax.sharding import PartitionSpec as P


MAXLEN = 4096
EPS = 1e-05
MIB = 1 << 20
LANES = 128
EARLY = (6, 5)
DIRECT = 4
BYTES = 1 << 26


VM = pl.BlockSpec(memory_space=pltpu.VMEM)
SM = pl.BlockSpec(memory_space=pltpu.SMEM)
HBM = pl.BlockSpec(memory_space=pltpu.HBM)
F32 = jnp.float32
BF16 = jnp.bfloat16


def gather_phases(count):
    bits = [1 << i for i in range(count.bit_length() - 1)][::-1]
    if len(bits) < 2:
        return [tuple(bits)] if bits else []
    low = bits[-1]
    rounds = [(bits[0] | low,)] if len(bits) > 1 else []
    middle = bits[1:-1]
    for at in range(0, len(middle), 2):
        pair = middle[at : at + 2]
        if len(pair) == 2:
            rounds.append((pair[0] | pair[1] | low, pair[1] | low, pair[0] | low))
        else:
            rounds.append((pair[0] | low,))
    return rounds + [(low,)]


def swap(value, mask):
    return lax.ppermute(value, "tp", [(s, s ^ mask) for s in range(lax.axis_size("tp"))])


def gather(value, held):
    *rounds, last = gather_phases(lax.axis_size("tp"))
    blocks, masks = value[None], [0]
    first = held[None]
    for number, group in enumerate(rounds):
        parts, before = [first if number == 0 else blocks], list(masks)
        for mask in group:
            parts.append(swap(blocks, mask))
            masks = masks + [m ^ mask for m in before]
        blocks = jnp.concatenate(parts, axis=0)
    far = swap(blocks, last[0])
    return blocks, far, masks, last[0]


def call(kernel, out_shape, in_specs, out_specs, scratch=(), aliases=None, limit=4, flops=1 << 20):
    return pl.pallas_call(
        kernel,
        out_shape=out_shape,
        in_specs=in_specs,
        out_specs=out_specs,
        scratch_shapes=scratch,
        input_output_aliases=aliases or {},
        compiler_params=pltpu.CompilerParams(vmem_limit_bytes=limit * MIB),
        cost_estimate=pl.CostEstimate(flops=flops, bytes_accessed=BYTES, transcendentals=0),
    )


def place(near, far, rows, masks, low):
    own = lax.axis_index("tp")
    for j, mask in enumerate(masks):
        rows[own ^ mask] = near[j]
        rows[own ^ mask ^ low] = far[j]


def joined(rows):
    return jnp.concatenate([rows[i] for i in range(rows.shape[0])], axis=1)


def dot(a, b):
    return jnp.dot(a, b, preferred_element_type=F32)


def heads_kernel(layer, masks, low, scale, near, far, gain, wq, wk, pair, normed, rows):
    place(near, far, rows, masks, low)
    x = joined(rows).astype(F32)
    inv = lax.rsqrt(jnp.mean(x * x, axis=1, keepdims=True) + EPS)
    n = (x * inv * gain[layer : layer + 1].astype(F32)).astype(BF16)
    normed[...] = n
    width = wq.shape[1]
    both = dot(n, jnp.concatenate([wq[...], wk[...]], axis=1))
    pair[0] = both[:, :width].astype(BF16)
    pair[1] = (both[:, width:] * scale).astype(BF16)


def as_column(row):
    n = row.shape[1]
    same = lax.broadcasted_iota(jnp.int32, (n, n), 0) == lax.broadcasted_iota(jnp.int32, (n, n), 1)
    return jnp.sum(jnp.where(same, row, 0.0), axis=1, keepdims=True)


def gates_kernel(
    layer, split, normed, wv, wo, wi, wf, ibias, fbias, slope, lengths, stab,
    values, outgate, factors, stab_new, columns, decays,
):
    n = normed[...]
    width = wv.shape[1]
    both = dot(n, jnp.concatenate([wv[...], wo[...]], axis=1))
    values[...] = both[:, :width].astype(BF16)
    outgate[...] = both[:, width:].astype(BF16)

    def logits(w):
        return lax.dot_general(w[layer], n, (((1,), (1,)), ((), ())), preferred_element_type=F32)

    row = slice(layer, layer + 1)
    position = lengths[...].astype(F32) / MAXLEN
    ingate = logits(wi) + as_column(ibias[row])
    forget = jax.nn.log_sigmoid(logits(wf) + as_column(fbias[row]) + as_column(slope[row]) * position)
    held = forget + stab[layer]
    top = jnp.maximum(held, ingate)
    stab_new[...] = top
    index = lax.broadcasted_iota(jnp.int32, top.shape, 0)
    mine = index == lax.axis_index("tp") // split
    decay = jnp.sum(jnp.where(mine, jnp.exp(held - top), 0.0), axis=0, keepdims=True)
    weight = jnp.sum(jnp.where(mine, jnp.exp(ingate - top), 0.0), axis=0, keepdims=True)
    factors[...] = jnp.where(index == 0, decay, weight).T
    batch, lanes = n.shape[0], columns.shape[1]
    v = both[:, :width].astype(BF16).astype(F32) * factors[:, 1:2]
    if lanes > batch:
        v = jnp.concatenate([v, jnp.zeros((lanes - batch, width), F32)], axis=0)
    columns[...] = v.T
    decays[...] = jnp.broadcast_to(factors[:, 0:1], decays.shape)


def in_order(parts, rows):
    local = lax.rem(lax.axis_index("tp"), len(parts))
    for mask, part in enumerate(parts):
        rows[local ^ mask] = part[...]


def read_kernel(layer, split, rows, memory, kept, *refs):
    pairs, refs = refs[:split], refs[split:]
    sums, refs = refs[:split], refs[split:]
    values, outgate, factors, gain, gated, sums_new, keys, rest, query, pieces, arrived = refs
    (first, width, depth), batch = kept.shape, values.shape[0]
    lanes = -(-batch // LANES) * LANES

    def fetch(i):
        part = pl.ds(i * rows, rows)
        return pltpu.make_async_copy(memory.at[layer, pl.ds(first + i * rows, rows)], rest.at[part], arrived.at[i])

    for i in range((batch - first) // rows):
        fetch(i).start()
    in_order(pairs, pieces)
    q = jnp.concatenate([pieces[i, 0] for i in range(split)], axis=1).astype(F32)
    query[...] = q
    key = jnp.concatenate([pieces[i, 1] for i in range(split)], axis=1).astype(F32)
    keys[...] = key
    lane = lax.broadcasted_iota(jnp.int32, (width, lanes), 1)

    ones = jnp.ones((LANES, LANES), BF16)
    direct = rows * DIRECT // 8

    def add(state, i, at, total):
        products = []
        for r in range(rows):
            x = state[i * rows + r] * query[pl.ds(at + i * rows + r, 1), :]
            products.append(sum(x[:, j : j + LANES] for j in range(0, depth, LANES)))
        if direct < rows:
            summed = dot(jnp.concatenate(products[direct:], axis=0).astype(BF16), ones)
        for r in range(rows):
            if r < direct:
                column = jnp.sum(products[r], axis=1, keepdims=True)
            else:
                column = summed[(r - direct) * width : (r - direct + 1) * width]
            total = jnp.where(lane == at + i * rows + r, column, total)
        return total

    def late(i, total):
        fetch(i).wait()
        return add(rest, i, first, total)

    total = jnp.zeros((width, lanes), F32)
    total = lax.fori_loop(0, first // rows, lambda i, total: add(kept, i, 0, total), total)
    total = lax.fori_loop(0, (batch - first) // rows, late, total)
    read = total.T[:batch]
    decay, weight = factors[:, 0:1], factors[:, 1:2]
    match = weight * jnp.sum(key * q, axis=1, keepdims=True)
    v = values[...].astype(F32)
    numerator = decay * read + match * v
    held = sum(s[layer] * p[0].astype(F32) for s, p in zip(sums, pairs))
    below = decay * jnp.sum(held, axis=1, keepdims=True) + match
    hidden = numerator / jnp.maximum(jnp.abs(below), 1.0)
    gate = jax.nn.sigmoid(outgate[...].astype(F32))
    gated[...] = (hidden * gain[layer : layer + 1].astype(F32) * gate).astype(BF16)
    sums_new[...] = decay * sums[0][layer] + weight * pairs[0][1].astype(F32)


def out_kernel(layer, masks, low, near, far, current, wo, after, rows):
    place(near, far, rows, masks, low)
    total = current[...].astype(F32) + dot(joined(rows), wo[layer])
    after[...] = total.astype(BF16)


def update_kernel(layer, start, count, rows, kept, rest, columns, decays, keys, _old, new, staged, sent):
    first, width, depth = kept.shape
    lanes = columns.shape[1]

    def send(i):
        part = pl.ds(i * rows, rows)
        return pltpu.make_async_copy(staged.at[part], new.at[layer, pl.ds(start + i * rows, rows)], sent.at[i])

    lane = lax.broadcasted_iota(jnp.int32, columns.shape, 1)
    direct = rows * DIRECT // 8
    operand = keys[...].astype(BF16)
    if lanes > keys.shape[0]:
        operand = jnp.concatenate([operand, jnp.zeros((lanes - keys.shape[0], depth), BF16)], axis=0)

    def some(state, skipped, i, carry):
        at = start + i * rows
        if direct < rows:
            chosen = [jnp.where(lane == at + r, columns[...], 0.0).astype(BF16) for r in range(direct, rows)]
            outer = dot(jnp.concatenate(chosen, axis=0), operand)
        if direct:
            turned = pltpu.roll(columns[...], lanes - at, axis=1)
        for r in range(rows):
            if r < direct:
                added = jnp.broadcast_to(turned[:, r : r + 1], (width, depth)) * keys[pl.ds(at + r, 1), :]
            else:
                added = outer[(r - direct) * width : (r - direct + 1) * width]
            staged[i * rows + r] = decays[pl.ds(at + r, 1), :] * state[at - skipped + r] + added
        send(i).start()
        return carry

    steps = count // rows
    middle = min(max((first - start) // rows, 0), steps)
    lax.fori_loop(0, middle, functools.partial(some, kept, 0), 0)
    lax.fori_loop(middle, steps, functools.partial(some, rest, first), 0)
    for i in range(steps):
        send(i).wait()


def store_kernel(blocks, *refs):
    parts, (sums, stab, sent) = refs[: 2 * blocks], refs[2 * blocks :]
    copies = []
    for i, part in enumerate(parts):
        target = sums.at[i] if i < blocks else stab.at[i - blocks]
        copies.append(pltpu.make_async_copy(part, target, sent.at[i]))
    for copy in copies:
        copy.start()
    for copy in copies:
        copy.wait()


def in_hbm(x):
    return pltpu.with_memory_space_constraint(x, pltpu.HBM)


def load_kernel(layer, whole, sliced, *refs):
    arrived, count = refs[-1], whole + sliced
    copies = []
    for i in range(count):
        source = refs[i] if i < whole else refs[i].at[layer]
        copies.append(pltpu.make_async_copy(source, refs[count + i], arrived.at[i]))
    for copy in copies:
        copy.start()
    for copy in copies:
        copy.wait()


def load(layer, whole, sliced):
    count = len(whole) + len(sliced)
    shapes = [a.shape for a in whole] + [a.shape[1:] for a in sliced]
    return call(
        functools.partial(load_kernel, layer, len(whole), len(sliced)),
        tuple(pltpu.VMEM(s, a.dtype) for s, a in zip(shapes, (*whole, *sliced))),
        [HBM] * count,
        (VM,) * count,
        [pltpu.SemaphoreType.DMA((count,))],
    )(*(in_hbm(a) for a in (*whole, *sliced)))


def state_kernel(layer, rows, memory, kept, arrived):
    copies = []
    for i in range(kept.shape[0] // rows):
        part = pl.ds(i * rows, rows)
        copies.append(pltpu.make_async_copy(memory.at[layer, part], kept.at[part], arrived.at[i]))
    for copy in copies:
        copy.start()
    for copy in copies:
        copy.wait()


def body(
    tokens,
    lengths,
    cell_memory,
    key_sums,
    stabilizer,
    norm_gain,
    query_weight,
    key_weight,
    value_weight,
    outgate_weight,
    ingate_weight,
    forget_weight,
    ingate_bias,
    forget_bias,
    forget_slope,
    head_gain,
    output_weight,
):
    count = lax.axis_size("tp")
    blocks, batch, width, depth = cell_memory.shape
    heads = stabilizer.shape[2]
    split = count // heads

    def pieces(value):
        found = [value]
        for mask in range(1, split):
            found.append(swap(value, mask))
        return found

    shape = jax.ShapeDtypeStruct
    rows = 8 if batch % 8 == 0 else 1
    lanes = -(-batch // LANES) * LANES
    sizes = (batch // rows // 2 * rows, batch - batch // rows // 2 * rows)
    weights = [query_weight, key_weight, value_weight, outgate_weight]
    own_sums, wi, wf, ibias, fbias, slope, at, stab, norm_gain, head_gain, current, *loaded = load(
        0,
        [
            key_sums,
            jnp.swapaxes(ingate_weight, 1, 2),
            jnp.swapaxes(forget_weight, 1, 2),
            ingate_bias,
            forget_bias,
            forget_slope,
            lengths[None],
            jnp.swapaxes(stabilizer, 1, 2),
            norm_gain,
            head_gain,
            tokens,
        ],
        weights,
    )
    near, far, masks, low = gather(tokens, current)
    sums = pieces(own_sums)
    loaded = [loaded]
    for layer in range(1, blocks):
        *outs, wq, wk, wv, wg = load(layer, [output_weight] if layer == 1 else [], weights)
        wo = outs[0] if outs else wo
        loaded.append([wq, wk, wv, wg])
    if blocks == 1:
        (wo,) = load(1, [output_weight], [])
    memory = in_hbm(cell_memory)
    new_memory, sums_out, stabs = at, [], []
    for layer in range(blocks):
        if layer:
            near, far, masks, low = gather(current, current)
        wq, wk, wv, wg = loaded[layer]
        first = batch // rows * EARLY[layer > 0] // 10 * rows
        kept = call(
            functools.partial(state_kernel, layer, rows),
            pltpu.VMEM((first, width, depth), F32),
            [HBM],
            VM,
            [pltpu.SemaphoreType.DMA((first // rows,))],
        )(memory)
        pair, normed = call(
            functools.partial(heads_kernel, layer, masks, low, depth ** (-0.5)),
            (shape((2, batch, width), BF16), pltpu.VMEM((batch, count * width), BF16)),
            [VM] * 5,
            (VM, VM),
            [pltpu.VMEM((count, batch, width), BF16)],
        )(near, far, norm_gain, wq, wk)
        pairs = pieces(pair)
        values, outgate, factors, new_stab, columns, decays = call(
            functools.partial(gates_kernel, layer, split),
            (
                shape((batch, width), BF16),
                shape((batch, width), BF16),
                shape((batch, heads), F32),
                pltpu.VMEM(stab.shape[1:], F32),
                pltpu.VMEM((width, lanes), F32),
                pltpu.VMEM((batch, depth), F32),
            ),
            [VM] * 10,
            (VM,) * 6,
        )(normed, wv, wg, wi, wf, ibias, fbias, slope, at, stab)
        stabs.append(new_stab)
        gated, new_sums, keys, rest = call(
            functools.partial(read_kernel, layer, split, rows),
            (
                shape((batch, width), BF16),
                pltpu.VMEM((batch, width), F32),
                pltpu.VMEM((batch, depth), F32),
                pltpu.VMEM((batch - first, width, depth), F32),
            ),
            [HBM] + [VM] * (5 + 2 * split),
            (VM,) * 4,
            [
                pltpu.VMEM((batch, depth), F32),
                pltpu.VMEM((split, 2, batch, width), BF16),
                pltpu.SemaphoreType.DMA(((batch - first) // rows,)),
            ],
        )(memory, kept, *pairs, *sums, values, outgate, factors, head_gain)
        sums_out.append(new_sums)

        near, far, masks, low = gather(gated, gated)
        for part, size in enumerate(sizes):
            new_memory = call(
                functools.partial(update_kernel, layer, part * sizes[0], size, rows),
                shape(cell_memory.shape, F32),
                [VM] * 5 + [HBM],
                HBM,
                [pltpu.VMEM((size, width, depth), F32), pltpu.SemaphoreType.DMA((size // rows,))],
                {} if layer == part == 0 else {5: 0},
                limit=8,
            )(kept, rest, columns, decays, keys, in_hbm(new_memory))

        current = call(
            functools.partial(out_kernel, layer, masks, low),
            shape((batch, width), BF16),
            [VM] * 4,
            VM,
            [pltpu.VMEM((count, batch, width), BF16)],
        )(near, far, current, wo)
    new_sums, new_stab = call(
        functools.partial(store_kernel, blocks),
        (shape(own_sums.shape, F32), shape(stab.shape, F32)),
        [VM] * (2 * blocks),
        (HBM, HBM),
        [pltpu.SemaphoreType.DMA((2 * blocks,))],
    )(*sums_out, *stabs)
    return current, new_memory, new_sums, jnp.swapaxes(new_stab, 1, 2)


def solution(mesh):
    in_specs = (
        P("grp", "tp"),
        P("grp"),
        P(None, "grp", "tp", None),
        P(None, "grp", "tp"),
        P(None, "grp", None),
        P(),
        P(None, None, "tp"),
        P(None, None, "tp"),
        P(None, None, "tp"),
        P(None, None, "tp"),
        P(),
        P(),
        P(),
        P(),
        P(),
        P(None, "tp"),
        P(None, None, "tp"),
    )
    out_specs = (
        P("grp", "tp"),
        P(None, "grp", "tp", None),
        P(None, "grp", "tp"),
        P(None, "grp", None),
    )

    return jax.shard_map(body, mesh=mesh, in_specs=in_specs, out_specs=out_specs, check_vma=False)
```
